32 devices in a mesh: fs: 16 (over z, y, x), tp: 2 (over core).
Axes of the slice: x: 2, y: 2, z: 4, core: 2. Of those that a mesh axis runs over, the one named last changes fastest.
Arguments:
- block_input: bfloat16 [16384, 2048], P('fs'), may hold values from -6 to 6
- value_cotangent: bfloat16 [16384, 1024], P('fs', 'tp'), may hold values from -6 to 6
- mixed_output: bfloat16 [16384, 1024], P('fs', 'tp'), may hold values from -6 to 6
- output_cotangent: bfloat16 [16384, 2048], P('fs'), may hold values from -6 to 6
- value_weight: float32 [2048, 1024], P('fs', 'tp'), may hold values from -0.125 to 0.125
- output_weight: float32 [1024, 2048], P('tp', 'fs'), may hold values from -0.1875 to 0.1875
- value_basis: bfloat16 [2048, 384], P('fs'), may hold values from -0.125 to 0.125
- output_basis: bfloat16 [2048, 384], P('fs'), may hold values from -0.125 to 0.125
- value_mean: float32 [384, 1024], P(None, 'tp'), may hold values from -4 to 4
- value_square: float32 [384, 1024], P(None, 'tp'), may hold values from 0.3 to 2
- output_mean: float32 [1024, 384], P('tp'), may hold values from -4 to 4
- output_square: float32 [1024, 384], P('tp'), may hold values from 0.3 to 2
Outputs:
- value_next: float32 [2048, 1024], P('fs', 'tp')
- value_copy: bfloat16 [2048, 1024], P(None, 'tp')
- value_step: float32 [2048, 1024], P('fs', 'tp')
- value_mean_next: float32 [384, 1024], P(None, 'tp')
- value_square_next: float32 [384, 1024], P(None, 'tp')
- output_next: float32 [1024, 2048], P('tp', 'fs')
- output_copy: bfloat16 [1024, 2048], P('tp')
- output_step: float32 [1024, 2048], P('tp', 'fs')
- output_mean_next: float32 [1024, 384], P('tp')
- output_square_next: float32 [1024, 384], P('tp')
The draws below stay inside these ranges and needn't reach their ends.
All inputs are finite; a program needn't handle non-finite values.
Results may differ from the reference program's by a relative error of at most 0.002.
Values may be sent and summed in bfloat16 or wider, within the bound.
A program may use at most 64 MiB of HBM per device.

```python
import math
import jax
import jax.numpy as jnp
from jax import lax

D = 2048
E = 1024
R = 384
TOKENS = 16384


def block_scale(own_key, dims, shards, smallest, high):
    loudness = 1.0
    for axis_at, parts in shards:
        draws = jax.random.uniform(jax.random.fold_in(jax.random.fold_in(own_key, 6), axis_at), (parts,), jnp.float32, smallest / len(shards), high / len(shards))
        loudness = loudness * jnp.repeat(jnp.exp(draws), dims[axis_at] // parts).reshape((-1,) + (1,) * (len(dims) - 1 - axis_at))
    return loudness


def normal_values(own_key, dims, spread, limit, pieces=(), kind=jnp.bfloat16):
    drawn = spread * jax.random.normal(own_key, dims, jnp.float32)
    if pieces:
        drawn = drawn * block_scale(own_key, dims, pieces, -0.22, 0.18)
    return jnp.clip(drawn, -limit, limit).astype(kind)


def setup_inputs(seed: int = 0) -> dict:
    keys = jax.random.split(jax.random.key(seed), 13)
    return {
        "block_input": normal_values(keys[0], (TOKENS, D), 1.0, 6.0, ((0, 16),)),
        "value_cotangent": normal_values(keys[1], (TOKENS, E), 1.0, 6.0, ((0, 16), (1, 2))),
        "mixed_output": normal_values(keys[2], (TOKENS, E), 1.0, 6.0, ((0, 16), (1, 2))),
        "output_cotangent": normal_values(keys[3], (TOKENS, D), 1.0, 6.0, ((0, 16),)),
        "value_weight": normal_values(keys[4], (D, E), D ** -0.5, 0.125, ((0, 16), (1, 2)), jnp.float32),
        "output_weight": normal_values(keys[5], (E, D), E ** -0.5, 0.1875, ((0, 2), (1, 16)), jnp.float32),
        "value_basis": normal_values(keys[6], (D, R), D ** -0.5, 0.125, ((0, 16),)),
        "output_basis": normal_values(keys[7], (D, R), D ** -0.5, 0.125, ((0, 16),)),
        "value_mean": normal_values(keys[8], (R, E), 0.7, 4.0, ((1, 2),), jnp.float32),
        "value_square": jnp.clip(jnp.exp(math.log(2.0) - 1.89712 * jax.random.uniform(keys[9], (R, E), jnp.float32) ** block_scale(keys[9], (R, E), ((1, 2),), -0.2, 0.2)), 0.3, 2.0),
        "output_mean": normal_values(keys[10], (E, R), 0.7, 4.0, ((0, 2),), jnp.float32),
        "output_square": jnp.clip(jnp.exp(math.log(2.0) - 1.89712 * jax.random.uniform(keys[11], (E, R), jnp.float32) ** block_scale(keys[11], (E, R), ((0, 2),), -0.2, 0.2)), 0.3, 2.0),
    }


def reference(block_input, value_cotangent, mixed_output, output_cotangent, value_weight, output_weight, value_basis, output_basis, value_mean, value_square, output_mean, output_square):
    highest = lax.Precision.HIGHEST
    scaling = 1.0 / math.sqrt(TOKENS)
    value_grad = jnp.dot(block_input.T, value_cotangent, preferred_element_type=jnp.float32)
    output_grad = jnp.dot(mixed_output.T, output_cotangent, preferred_element_type=jnp.float32)
    value_base = value_basis.astype(jnp.float32)
    output_base = output_basis.astype(jnp.float32)
    value_low = jnp.dot(value_base.T, value_grad, precision=highest) * scaling
    output_low = jnp.dot(output_grad, output_base, precision=highest) * scaling
    total_squares = jnp.sum(value_low * value_low) + jnp.sum(output_low * output_low)
    clip_scale = 1.0 / jnp.sqrt(1.0 + total_squares / (2.0 * R * E))
    value_scaled = clip_scale * value_low
    output_scaled = clip_scale * output_low
    value_mean_next = 0.8 * value_mean + 0.2 * value_scaled
    output_mean_next = 0.8 * output_mean + 0.2 * output_scaled
    value_square_next = 0.9 * value_square + 0.1 * value_scaled * value_scaled
    output_square_next = 0.9 * output_square + 0.1 * output_scaled * output_scaled
    value_norm = value_mean_next / jnp.sqrt(value_square_next + 0.1)
    output_norm = output_mean_next / jnp.sqrt(output_square_next + 0.1)
    value_step = jnp.dot(value_base, value_norm, precision=highest)
    output_step = jnp.dot(output_norm, output_base.T, precision=highest)
    value_next = value_weight - 0.02 * value_step
    output_next = output_weight - 0.02 * output_step
    return (value_next, value_next.astype(jnp.bfloat16), value_step, value_mean_next, value_square_next, output_next, output_next.astype(jnp.bfloat16), output_step, output_mean_next, output_square_next)
```

```python
import functools
import math

import jax
import jax.numpy as jnp
from jax import lax
from jax.experimental import pallas as pl
from jax.experimental.pallas import tpu as pltpu
from jax.sharding import PartitionSpec as P

MESH = pl.DeviceIdType.MESH
VALUE_RATE = 125.0 / 0.125
OUTPUT_RATE = 125.0 / 0.1875
TOKEN_TILE = 256


def split_fs(n):
    inner = 2 if n % 2 == 0 else 1
    middle = 2 if n % (2 * inner) == 0 else 1
    return n // (inner * middle), middle, inner


class Place:
    def __init__(self, n):
        self.sizes = split_fs(n)
        self.me = lax.axis_index("fs")
        self.core = lax.axis_index("tp")
        self.par = lax.rem(self.core, 2)
        _, b, c = self.sizes
        self.z = self.me // (b * c)
        self.y = lax.rem(self.me // c, b)
        self.x = lax.rem(self.me, c)

    def at(self, dz, ds, dt, par=None):
        a, b, c = self.sizes
        par = self.par if par is None else par
        dy = ds * (1 - par) + dt * par
        dx = ds * par + dt * (1 - par)
        z = lax.rem(self.z + dz + a, a)
        y = lax.rem(self.y + dy, b)
        x = lax.rem(self.x + dx, c)
        return (z * b + y) * c + x


class Gather:
    def __init__(self, place, slots, send, recv):
        self.p, self.slots, self.send, self.recv = place, slots, send, recv
        self.a = place.sizes[0]
        self.started = []

    def copy(self, j, src, to, sid, rid):
        ref = self.slots[j](src)
        return pltpu.make_async_remote_copy(
            src_ref=ref, dst_ref=ref, send_sem=self.send.at[j, sid], recv_sem=self.recv.at[j, rid],
            device_id={"fs": to}, device_id_type=MESH)

    def rel(self, dz, ds, dt):
        return (dz * 2 + ds) * 2 + dt

    def go(self, j, src, to, sid, rid):
        c = self.copy(j, src, to, sid, rid)
        c.start()
        self.started.append(c)

    def arrive(self, dz, ds, dt):
        for j in range(len(self.slots)):
            src = self.p.at(-dz, ds, dt)
            self.copy(j, src, self.p.me, 0, self.rel(dz, ds, dt)).wait_recv()

    def to_s(self, dz):
        for j in range(len(self.slots)):
            self.go(j, self.p.at(-dz, 0, 0), self.p.at(0, 1, 0), self.a + dz, self.rel(dz, 1, 0))

    def to_t(self, dz, ds):
        for j in range(len(self.slots)):
            self.go(j, self.p.at(-dz, ds, 0), self.p.at(0, 0, 1), 2 * self.a + dz * 2 + ds, self.rel(dz, ds, 1))

    def begin(self):
        for dz in range(1, self.a):
            for j in range(len(self.slots)):
                self.go(j, self.p.me, self.p.at(dz, 0, 0), dz, self.rel(dz, 0, 0))
        self.to_s(0)
        self.to_t(0, 0)

    def stage_z(self, seen=lambda *k: None):
        for dz in range(1, self.a):
            self.arrive(dz, 0, 0)
            self.to_s(dz)
            self.to_t(dz, 0)
            seen(dz, 0, 0)

    def stage_s(self, seen=lambda *k: None):
        for dz in range(self.a):
            self.arrive(dz, 1, 0)
            self.to_t(dz, 1)
            seen(dz, 1, 0)

    def stage_t(self, seen=lambda *k: None):
        for dz in range(self.a):
            for ds in range(2):
                self.arrive(dz, ds, 1)
                seen(dz, ds, 1)

    def finish(self):
        for c in self.started:
            c.wait_send()


def exchange(n, scaling, x_hbm, v_hbm, m_hbm, o_hbm, vb_ref, ob_ref, vw_ref, ow_ref,
             bases, wv, wo, low_v, low_o,
             x_ref, v_ref, m_ref, o_ref, acc_v, acc_o, part_v, part_o, got_v, got_o,
             load_sem, own_sem, b_send, b_recv, c_send, c_recv, w_send, w_recv, l_send, l_recv, r_send, r_recv):
    p = Place(n)
    a = p.sizes[0]
    par, me = p.par, p.me
    loads = [pltpu.make_async_copy(s, d, load_sem.at[i]) for i, (s, d) in enumerate(
        ((x_hbm, x_ref), (v_hbm, v_ref), (o_hbm, o_ref), (m_hbm, m_ref)))]
    own = [pltpu.make_async_copy(s, d, own_sem.at[i]) for i, (s, d) in enumerate(
        ((vb_ref, bases.at[0, me]), (ob_ref, bases.at[1, me]), (vw_ref, wv.at[me]), (ow_ref, wo.at[me])))]
    for c in own + loads:
        c.start()
    partner = p.core + 1 - 2 * par
    barrier = pltpu.get_barrier_semaphore()
    peers = [p.at(dz, 0, 0) for dz in range(1, a)] + [p.at(0, 1, 0), p.at(0, 0, 1)]
    for to in peers:
        pl.semaphore_signal(barrier, inc=1, device_id={"fs": to}, device_id_type=MESH)
    pl.semaphore_signal(barrier, inc=1, device_id={"tp": partner}, device_id_type=MESH)
    pl.semaphore_wait(barrier, len(peers) + 1)
    for c in own:
        c.wait()

    crossed = []

    def cross(dz, ds, dt):
        k = (dz * 2 + ds) * 2 + dt
        ref = bases.at[par, p.at(-dz, ds, dt)]
        c = pltpu.make_async_remote_copy(
            src_ref=ref, dst_ref=ref, send_sem=c_send.at[k], recv_sem=c_recv.at[k],
            device_id={"tp": partner}, device_id_type=MESH)
        c.start()
        crossed.append(c)

    gb = Gather(p, [lambda i: bases.at[par, i]], b_send, b_recv)
    gb.begin()
    gb.stage_z(cross)
    gb.stage_s(cross)
    gb.stage_t(cross)
    gw = Gather(p, [lambda i: wv.at[i], lambda i: wo.at[i]], w_send, w_recv)
    gw.begin()
    for dz in range(a):
        for ds in range(2):
            for dt in range(2):
                k = (dz * 2 + ds) * 2 + dt
                if k:
                    ref = bases.at[1 - par, p.at(-dz, ds, dt, 1 - par)]
                    pltpu.make_async_remote_copy(
                        src_ref=ref, dst_ref=ref, send_sem=c_send.at[k], recv_sem=c_recv.at[k],
                        device_id={"tp": partner}, device_id_type=MESH).wait_recv()
    for c in loads:
        c.wait()

    depth, rank = bases.shape[2], bases.shape[3]
    tokens = x_ref.shape[0]
    tile = math.gcd(tokens, TOKEN_TILE)
    acc_v[...] = jnp.zeros_like(acc_v)
    acc_o[...] = jnp.zeros_like(acc_o)
    whole_v = bases[0].reshape(n * depth, rank)
    whole_o = bases[1].reshape(n * depth, rank)
    first = (((0,), (0,)), ((), ()))

    def halves(value):
        high = value.astype(jnp.bfloat16)
        return high, (value - high.astype(jnp.float32)).astype(jnp.bfloat16)

    @pl.loop(0, tokens // tile)
    def _(step):
        rows = pl.ds(pl.multiple_of(step * tile, tile), tile)
        cot = v_ref[rows, :]
        for half in halves(jnp.dot(x_ref[rows, :], whole_v, preferred_element_type=jnp.float32)):
            acc_v[...] += lax.dot_general(half, cot, first, preferred_element_type=jnp.float32)
        mixed = m_ref[rows, :]
        for half in halves(jnp.dot(o_ref[rows, :], whole_o, preferred_element_type=jnp.float32)):
            acc_o[...] += lax.dot_general(mixed, half, first, preferred_element_type=jnp.float32)

    parts, gots = (part_v, part_o), (got_v, got_o)
    for part, acc in ((part_v, acc_v), (part_o, acc_o)):
        high = part.shape[1]
        for i in range(n):
            part[i] = acc[i * high:(i + 1) * high, :] * scaling

    sent = []

    def hand(block, to, slot):
        for j in range(2):
            c = pltpu.make_async_remote_copy(
                src_ref=parts[j].at[block], dst_ref=gots[j].at[slot],
                send_sem=r_send.at[j, slot], recv_sem=r_recv.at[j, slot],
                device_id={"fs": to}, device_id_type=MESH)
            c.start()
            sent.append(c)

    def take(block, slot):
        for j in range(2):
            pltpu.make_async_remote_copy(
                src_ref=parts[j].at[block], dst_ref=gots[j].at[slot],
                send_sem=r_send.at[j, slot], recv_sem=r_recv.at[j, slot],
                device_id={"fs": me}, device_id_type=MESH).wait_recv()
            parts[j][block] += gots[j][slot]

    order = list(range(1, a)) + [0]
    for dz in order:
        for ds in (1, 0):
            hand(p.at(dz, ds, 1), p.at(0, 0, 1), dz * 2 + ds)
    for dz in order:
        take(p.at(dz, 1, 0), dz * 2 + 1)
        hand(p.at(dz, 1, 0), p.at(0, 1, 0), 2 * a + dz)
        take(p.at(dz, 0, 0), dz * 2)
    for dz in order:
        take(p.at(dz, 0, 0), 2 * a + dz)
        if dz:
            hand(p.at(dz, 0, 0), p.at(dz, 0, 0), 3 * a + dz)
    gw.stage_z()
    for dz in range(1, a):
        take(me, 3 * a + dz)
    low_v[me] = part_v[me]
    low_o[me] = part_o[me]
    gl = Gather(p, [lambda i: low_v.at[i], lambda i: low_o.at[i]], l_send, l_recv)
    gl.begin()
    gl.stage_z()
    gl.stage_s()
    gl.stage_t()
    gw.stage_s()
    gw.stage_t()
    for c in crossed + sent:
        c.wait_send()
    gb.finish()
    gw.finish()
    gl.finish()


def low_and_weights(block_input, value_cotangent, mixed_output, output_cotangent, value_basis, output_basis, vw_code, ow_code):
    n = lax.axis_size("fs")
    depth, rank = value_basis.shape
    tokens, width = value_cotangent.shape
    wide = block_input.shape[1]
    a = split_fs(n)[0]
    scaling = 1.0 / math.sqrt(tokens * n)
    f32, b16 = jnp.float32, jnp.bfloat16
    rv, ro = rank // n, width // n
    vmem = pl.BlockSpec(memory_space=pltpu.VMEM)
    hbm = pl.BlockSpec(memory_space=pl.ANY)
    dma = pltpu.SemaphoreType.DMA
    return pl.pallas_call(
        functools.partial(exchange, n, scaling),
        out_shape=(
            jax.ShapeDtypeStruct((2, n, depth, rank), b16),
            jax.ShapeDtypeStruct((n,) + vw_code.shape, vw_code.dtype),
            jax.ShapeDtypeStruct((n,) + ow_code.shape, ow_code.dtype),
            jax.ShapeDtypeStruct((n, rv, width), f32),
            jax.ShapeDtypeStruct((n, ro, rank), f32),
        ),
        in_specs=[hbm] * 4 + [vmem] * 4,
        out_specs=[vmem] * 5,
        scratch_shapes=[
            pltpu.VMEM((tokens, wide), b16), pltpu.VMEM((tokens, width), b16),
            pltpu.VMEM((tokens, width), b16), pltpu.VMEM((tokens, wide), b16),
            pltpu.VMEM((rank, width), f32), pltpu.VMEM((width, rank), f32),
            pltpu.VMEM((n, rv, width), f32), pltpu.VMEM((n, ro, rank), f32),
            pltpu.VMEM((4 * a, rv, width), f32), pltpu.VMEM((4 * a, ro, rank), f32),
            dma((4,)), dma((4,)),
            dma((1, 4 * a)), dma((1, 4 * a)), dma((4 * a,)), dma((4 * a,)),
            dma((2, 4 * a)), dma((2, 4 * a)), dma((2, 4 * a)), dma((2, 4 * a)), dma((2, 4 * a)), dma((2, 4 * a)),
        ],
        compiler_params=pltpu.CompilerParams(
            collective_id=0, has_side_effects=True, vmem_limit_bytes=60 * 1024 * 1024),
    )(block_input, value_cotangent, mixed_output, output_cotangent, value_basis, output_basis, vw_code, ow_code)


def stepped(norm, basis, flip):
    high = norm.astype(jnp.bfloat16)
    low = (norm - high.astype(jnp.float32)).astype(jnp.bfloat16)
    if flip:
        return sum(lax.dot_general(h, basis, (((1,), (1,)), ((), ())), preferred_element_type=jnp.float32) for h in (high, low))
    return sum(jnp.dot(basis, h, preferred_element_type=jnp.float32) for h in (high, low))


def on_device(
    block_input,
    value_cotangent,
    mixed_output,
    output_cotangent,
    value_weight,
    output_weight,
    value_basis,
    output_basis,
    value_mean,
    value_square,
    output_mean,
    output_square,
):
    rank_size = value_basis.shape[1]
    local_width = value_cotangent.shape[1]
    wide = block_input.shape[1]
    bases, wv, wo, value_low, output_low = low_and_weights(
        block_input, value_cotangent, mixed_output, output_cotangent, value_basis, output_basis,
        jnp.exp2(VALUE_RATE * value_weight).astype(jnp.bfloat16),
        jnp.exp2(OUTPUT_RATE * output_weight).astype(jnp.bfloat16))
    value_low = value_low.reshape(rank_size, local_width)
    output_low = output_low.reshape(local_width, rank_size)
    squares = lax.psum(jnp.sum(value_low * value_low) + jnp.sum(output_low * output_low), "tp")
    entries = 2.0 * rank_size * local_width * lax.axis_size("tp")
    clip_scale = 1.0 / jnp.sqrt(1.0 + squares / entries)
    value_scaled = clip_scale * value_low
    output_scaled = clip_scale * output_low
    value_mean_next = 0.8 * value_mean + 0.2 * value_scaled
    output_mean_next = 0.8 * output_mean + 0.2 * output_scaled
    value_square_next = 0.9 * value_square + 0.1 * value_scaled * value_scaled
    output_square_next = 0.9 * output_square + 0.1 * output_scaled * output_scaled
    value_norm = value_mean_next / jnp.sqrt(value_square_next + 0.1)
    output_norm = output_mean_next / jnp.sqrt(output_square_next + 0.1)
    value_step = stepped(value_norm, value_basis, False)
    output_step = stepped(output_norm, output_basis, True)
    value_next = value_weight - 0.02 * value_step
    output_next = output_weight - 0.02 * output_step
    value_all = stepped(value_norm, bases[0].reshape(wide, rank_size), False)
    output_all = stepped(output_norm, bases[1].reshape(wide, rank_size), True)
    value_old = jnp.log2(wv.reshape(wide, local_width).astype(jnp.float32)) * (1.0 / VALUE_RATE)
    value_copy = (value_old - 0.02 * value_all).astype(jnp.bfloat16)
    output_old = jnp.log2(wo.transpose(1, 0, 2).reshape(local_width, wide).astype(jnp.float32)) * (1.0 / OUTPUT_RATE)
    output_copy = (output_old - 0.02 * output_all).astype(jnp.bfloat16)
    return (
        value_next,
        value_copy,
        value_step,
        value_mean_next,
        value_square_next,
        output_next,
        output_copy,
        output_step,
        output_mean_next,
        output_square_next,
    )


def solution(mesh):
    placed = (
        P("fs", None),
        P("fs", "tp"),
        P("fs", "tp"),
        P("fs", None),
        P("fs", "tp"),
        P("tp", "fs"),
        P("fs", None),
        P("fs", None),
        P(None, "tp"),
        P(None, "tp"),
        P("tp", None),
        P("tp", None),
    )
    return jax.shard_map(
        on_device,
        mesh=mesh,
        in_specs=placed,
        out_specs=(
            P("fs", "tp"),
            P(None, "tp"),
            P("fs", "tp"),
            P(None, "tp"),
            P(None, "tp"),
            P("tp", "fs"),
            P("tp", None),
            P("tp", "fs"),
            P("tp", None),
            P("tp", None),
        ),
        check_vma=False,
    )
```

```python
import functools
import math

import jax
import jax.numpy as jnp
from jax import lax
from jax.experimental import pallas as pl
from jax.experimental.pallas import tpu as pltpu
from jax.sharding import PartitionSpec as P

MESH = pl.DeviceIdType.MESH
VALUE_RATE = 125.0 / 0.125
OUTPUT_RATE = 125.0 / 0.1875
LOW_RATE = 124.0
BLOCK_LANES = 256
TOKEN_TILE = 256


def split_fs(n):
    inner = 2 if n % 2 == 0 else 1
    middle = 2 if n % (2 * inner) == 0 else 1
    return n // (inner * middle), middle, inner


class Place:
    def __init__(self, n):
        self.sizes = split_fs(n)
        self.me = lax.axis_index("fs")
        self.core = lax.axis_index("tp")
        self.par = lax.rem(self.core, 2)
        _, b, c = self.sizes
        self.z = self.me // (b * c)
        self.y = lax.rem(self.me // c, b)
        self.x = lax.rem(self.me, c)

    def at(self, dz, ds, dt, par=None):
        a, b, c = self.sizes
        par = self.par if par is None else par
        dy = ds * (1 - par) + dt * par
        dx = ds * par + dt * (1 - par)
        z = lax.rem(self.z + dz + a, a)
        y = lax.rem(self.y + dy, b)
        x = lax.rem(self.x + dx, c)
        return (z * b + y) * c + x


class Gather:
    def __init__(self, place, slots, send, recv):
        self.p, self.slots, self.send, self.recv = place, slots, send, recv
        self.a = place.sizes[0]
        self.started = []

    def copy(self, j, src, to, sid, rid):
        ref = self.slots[j](src)
        return pltpu.make_async_remote_copy(
            src_ref=ref, dst_ref=ref, send_sem=self.send.at[j, sid], recv_sem=self.recv.at[j, rid],
            device_id={"fs": to}, device_id_type=MESH)

    def rel(self, dz, ds, dt):
        return (dz * 2 + ds) * 2 + dt

    def go(self, j, src, to, sid, rid):
        c = self.copy(j, src, to, sid, rid)
        c.start()
        self.started.append(c)

    def arrive(self, dz, ds, dt):
        for j in range(len(self.slots)):
            src = self.p.at(-dz, ds, dt)
            self.copy(j, src, self.p.me, 0, self.rel(dz, ds, dt)).wait_recv()

    def to_s(self, dz):
        for j in range(len(self.slots)):
            self.go(j, self.p.at(-dz, 0, 0), self.p.at(0, 1, 0), self.a + dz, self.rel(dz, 1, 0))

    def to_t(self, dz, ds):
        for j in range(len(self.slots)):
            self.go(j, self.p.at(-dz, ds, 0), self.p.at(0, 0, 1), 2 * self.a + dz * 2 + ds, self.rel(dz, ds, 1))

    def begin(self):
        for dz in range(1, self.a):
            for j in range(len(self.slots)):
                self.go(j, self.p.me, self.p.at(dz, 0, 0), dz, self.rel(dz, 0, 0))
        self.to_s(0)
        self.to_t(0, 0)

    def stage_z(self, seen=lambda *k: None):
        for dz in range(1, self.a):
            self.arrive(dz, 0, 0)
            self.to_s(dz)
            self.to_t(dz, 0)
            seen(dz, 0, 0)

    def stage_s(self, seen=lambda *k: None):
        for dz in range(self.a):
            self.arrive(dz, 1, 0)
            self.to_t(dz, 1)
            seen(dz, 1, 0)

    def stage_t(self, seen=lambda *k: None):
        for dz in range(self.a):
            for ds in range(2):
                self.arrive(dz, ds, 1)
                seen(dz, ds, 1)

    def finish(self):
        for c in self.started:
            c.wait_send()


def exchange(n, scaling, x_hbm, v_hbm, m_hbm, o_hbm, vb_ref, ob_ref, vw_ref, ow_ref,
             bases, wv, wo, low_v, low_o, sums,
             vw32, ow32, x_ref, v_ref, m_ref, o_ref, acc_v, acc_o, part_v, part_o, got_v, got_o,
             load_sem, own_sem, b_send, b_recv, c_send, c_recv, w_send, w_recv, l_send, l_recv, r_send, r_recv, q_send, q_recv):
    p = Place(n)
    a = p.sizes[0]
    par, me = p.par, p.me
    loads = [pltpu.make_async_copy(s, d, load_sem.at[i]) for i, (s, d) in enumerate(
        ((vw_ref, vw32), (ow_ref, ow32), (x_hbm, x_ref), (v_hbm, v_ref), (o_hbm, o_ref), (m_hbm, m_ref)))]
    own = [pltpu.make_async_copy(s, d, own_sem.at[i]) for i, (s, d) in enumerate(
        ((vb_ref, bases.at[0, me]), (ob_ref, bases.at[1, me])))]
    for c in own + loads:
        c.start()
    partner = p.core + 1 - 2 * par
    barrier = pltpu.get_barrier_semaphore()
    peers = [p.at(dz, 0, 0) for dz in range(1, a)] + [p.at(0, 1, 0), p.at(0, 0, 1)]
    for to in peers:
        pl.semaphore_signal(barrier, inc=1, device_id={"fs": to}, device_id_type=MESH)
    cores = lax.axis_size("tp")
    siblings = [lax.rem(p.core + d, cores) for d in range(1, cores)]
    for to in siblings:
        pl.semaphore_signal(barrier, inc=1, device_id={"tp": to}, device_id_type=MESH)
    pl.semaphore_wait(barrier, len(peers) + len(siblings))
    for c in own:
        c.wait()

    crossed = []

    def cross(dz, ds, dt):
        k = (dz * 2 + ds) * 2 + dt
        ref = bases.at[par, p.at(-dz, ds, dt)]
        c = pltpu.make_async_remote_copy(
            src_ref=ref, dst_ref=ref, send_sem=c_send.at[k], recv_sem=c_recv.at[k],
            device_id={"tp": partner}, device_id_type=MESH)
        c.start()
        crossed.append(c)

    gb = Gather(p, [lambda i: bases.at[par, i]], b_send, b_recv)
    gb.begin()
    for c in loads[:2]:
        c.wait()
    wv[me] = jnp.exp2(VALUE_RATE * vw32[...]).astype(wv.dtype)
    wo[me] = jnp.exp2(OUTPUT_RATE * ow32[...]).astype(wo.dtype)
    gb.stage_z(cross)
    gb.stage_s(cross)
    gb.stage_t(cross)
    gw = Gather(p, [lambda i: wv.at[i], lambda i: wo.at[i]], w_send, w_recv)
    gw.begin()
    for dz in range(a):
        for ds in range(2):
            for dt in range(2):
                k = (dz * 2 + ds) * 2 + dt
                if k:
                    ref = bases.at[1 - par, p.at(-dz, ds, dt, 1 - par)]
                    pltpu.make_async_remote_copy(
                        src_ref=ref, dst_ref=ref, send_sem=c_send.at[k], recv_sem=c_recv.at[k],
                        device_id={"tp": partner}, device_id_type=MESH).wait_recv()
    for c in loads[2:]:
        c.wait()

    depth, rank = bases.shape[2], bases.shape[3]
    tokens = x_ref.shape[0]
    tile = math.gcd(tokens, TOKEN_TILE)
    acc_v[...] = jnp.zeros_like(acc_v)
    acc_o[...] = jnp.zeros_like(acc_o)
    whole_v = bases[0].reshape(n * depth, rank)
    whole_o = bases[1].reshape(n * depth, rank)
    first = (((0,), (0,)), ((), ()))

    def halves(value):
        high = value.astype(jnp.bfloat16)
        return high, (value - high.astype(jnp.float32)).astype(jnp.bfloat16)

    @pl.loop(0, tokens // tile)
    def _(step):
        rows = pl.ds(pl.multiple_of(step * tile, tile), tile)
        cot = v_ref[rows, :]
        for half in halves(jnp.dot(x_ref[rows, :], whole_v, preferred_element_type=jnp.float32)):
            acc_v[...] += lax.dot_general(half, cot, first, preferred_element_type=jnp.float32)
        mixed = m_ref[rows, :]
        for half in halves(jnp.dot(o_ref[rows, :], whole_o, preferred_element_type=jnp.float32)):
            acc_o[...] += lax.dot_general(mixed, half, first, preferred_element_type=jnp.float32)

    parts, gots = (part_v, part_o), (got_v, got_o)
    for part, acc in ((part_v, acc_v), (part_o, acc_o)):
        high = part.shape[1]
        for i in range(n):
            part[i] = acc[i * high:(i + 1) * high, :] * scaling

    sent = []

    def hand(block, to, slot):
        for j in range(2):
            c = pltpu.make_async_remote_copy(
                src_ref=parts[j].at[block], dst_ref=gots[j].at[slot],
                send_sem=r_send.at[j, slot], recv_sem=r_recv.at[j, slot],
                device_id={"fs": to}, device_id_type=MESH)
            c.start()
            sent.append(c)

    def take(block, slot):
        for j in range(2):
            pltpu.make_async_remote_copy(
                src_ref=parts[j].at[block], dst_ref=gots[j].at[slot],
                send_sem=r_send.at[j, slot], recv_sem=r_recv.at[j, slot],
                device_id={"fs": me}, device_id_type=MESH).wait_recv()
            parts[j][block] += gots[j][slot]

    order = list(range(1, a)) + [0]
    for dz in order:
        for ds in (1, 0):
            hand(p.at(dz, ds, 1), p.at(0, 0, 1), dz * 2 + ds)
    for dz in order:
        take(p.at(dz, 1, 0), dz * 2 + 1)
        hand(p.at(dz, 1, 0), p.at(0, 1, 0), 2 * a + dz)
        take(p.at(dz, 0, 0), dz * 2)
    for dz in order:
        take(p.at(dz, 0, 0), 2 * a + dz)
        if dz:
            hand(p.at(dz, 0, 0), p.at(dz, 0, 0), 3 * a + dz)
    gw.stage_z()
    for dz in range(1, a):
        take(me, 3 * a + dz)
    mine_v, mine_o = part_v[me], part_o[me]

    def one(reduce, value):
        return reduce(reduce(value, axis=1, keepdims=True), axis=0, keepdims=True)

    top = jnp.maximum(one(jnp.max, jnp.abs(mine_v)), one(jnp.max, jnp.abs(mine_o)))
    top = jnp.maximum(top * 1.01, 1e-30).astype(low_v.dtype)
    square = one(jnp.sum, mine_v * mine_v) + one(jnp.sum, mine_o * mine_o)
    rate = LOW_RATE / top.astype(jnp.float32)
    high = mine_v.shape[0]
    pad = low_v.shape[1] - high
    square_high, square_low = halves(square)
    row = lax.broadcasted_iota(jnp.int32, (pad, mine_v.shape[1]), 0)
    extra = jnp.where(row == 0, top.astype(jnp.float32), jnp.where(
        row == 1, square_high.astype(jnp.float32), square_low.astype(jnp.float32)))
    low_v[me] = jnp.concatenate([jnp.exp2(rate * mine_v), extra], axis=0).astype(low_v.dtype)
    low_o[me] = jnp.exp2(rate * mine_o).astype(low_o.dtype)
    gl = Gather(p, [lambda i: low_v.at[i], lambda i: low_o.at[i]], l_send, l_recv)
    gl.begin()
    gl.stage_z()
    gl.stage_s()
    gl.stage_t()
    total = jnp.zeros((1, 128), jnp.float32)
    for i in range(n):
        tail = low_v[i].astype(jnp.float32)
        total += tail[high + 1:high + 2, :128] + tail[high + 2:high + 3, :128]
    sums[p.core] = jnp.broadcast_to(total, sums.shape[1:])
    for d, to in enumerate(siblings):
        c = pltpu.make_async_remote_copy(
            src_ref=sums.at[p.core], dst_ref=sums.at[p.core], send_sem=q_send.at[d], recv_sem=q_recv.at[d],
            device_id={"tp": to}, device_id_type=MESH)
        c.start()
        sent.append(c)
    gw.stage_s()
    gw.stage_t()
    for d in range(cores - 1):
        ref = sums.at[lax.rem(p.core - d - 1 + cores, cores)]
        pltpu.make_async_remote_copy(
            src_ref=ref, dst_ref=ref, send_sem=q_send.at[d], recv_sem=q_recv.at[d],
            device_id={"tp": partner}, device_id_type=MESH).wait_recv()
    for c in crossed + sent:
        c.wait_send()
    gb.finish()
    gw.finish()
    gl.finish()


def low_and_weights(block_input, value_cotangent, mixed_output, output_cotangent, value_basis, output_basis, value_weight, output_weight):
    n = lax.axis_size("fs")
    depth, rank = value_basis.shape
    tokens, width = value_cotangent.shape
    wide = block_input.shape[1]
    a = split_fs(n)[0]
    cores = lax.axis_size("tp")
    scaling = 1.0 / math.sqrt(tokens * n)
    f32, b16 = jnp.float32, jnp.bfloat16
    rv, ro = rank // n, width // n
    vmem = pl.BlockSpec(memory_space=pltpu.VMEM)
    hbm = pl.BlockSpec(memory_space=pl.ANY)
    dma = pltpu.SemaphoreType.DMA
    return pl.pallas_call(
        functools.partial(exchange, n, scaling),
        out_shape=(
            jax.ShapeDtypeStruct((2, n, depth, rank), b16),
            jax.ShapeDtypeStruct((n,) + value_weight.shape, b16),
            jax.ShapeDtypeStruct((n,) + output_weight.shape, b16),
            jax.ShapeDtypeStruct((n, (rv + 18) // 16 * 16, width), b16),
            jax.ShapeDtypeStruct((n, ro, rank), b16),
            jax.ShapeDtypeStruct((cores, 8, 128), f32),
        ),
        in_specs=[hbm] * 4 + [hbm] * 4,
        out_specs=[vmem] * 6,
        scratch_shapes=[
            pltpu.VMEM(value_weight.shape, f32), pltpu.VMEM(output_weight.shape, f32),
            pltpu.VMEM((tokens, wide), b16), pltpu.VMEM((tokens, width), b16),
            pltpu.VMEM((tokens, width), b16), pltpu.VMEM((tokens, wide), b16),
            pltpu.VMEM((rank, width), f32), pltpu.VMEM((width, rank), f32),
            pltpu.VMEM((n, rv, width), f32), pltpu.VMEM((n, ro, rank), f32),
            pltpu.VMEM((4 * a, rv, width), f32), pltpu.VMEM((4 * a, ro, rank), f32),
            dma((6,)), dma((2,)),
            dma((1, 4 * a)), dma((1, 4 * a)), dma((4 * a,)), dma((4 * a,)),
            dma((2, 4 * a)), dma((2, 4 * a)), dma((2, 4 * a)), dma((2, 4 * a)), dma((2, 4 * a)), dma((2, 4 * a)),
            dma((cores,)), dma((cores,)),
        ],
        compiler_params=pltpu.CompilerParams(
            collective_id=0, has_side_effects=True, vmem_limit_bytes=60 * 1024 * 1024),
    )(block_input, value_cotangent, mixed_output, output_cotangent, value_basis, output_basis, value_weight, output_weight)


def split_norm(norm, norms):
    norms[0] = norm.astype(jnp.bfloat16)
    norms[1] = (norm - norms[0].astype(jnp.float32)).astype(jnp.bfloat16)


def value_steps(basis, norms):
    return (jnp.dot(basis, norms[0], preferred_element_type=jnp.float32)
            + jnp.dot(basis, norms[1], preferred_element_type=jnp.float32))


def output_steps(basis, norms):
    last = (((1,), (1,)), ((), ()))
    return (lax.dot_general(norms[0], basis, last, preferred_element_type=jnp.float32)
            + lax.dot_general(norms[1], basis, last, preferred_element_type=jnp.float32))


def epilogue(entries, low_v, low_o, sums, vm, vs, om, os, vw, ow, vb, ob, bases, wv, wo,
             v_next, v_copy, v_step, vm_next, vs_next, o_next, o_copy, o_step, om_next, os_next,
             norms_v, norms_o):
    @pl.when(pl.program_id(0) == 0)
    def _():
        n, high, high_o = low_v.shape[0], vm.shape[0] // low_v.shape[0], low_o.shape[1]
        total = sums[0, :1, :1]
        for i in range(1, sums.shape[0]):
            total += sums[i, :1, :1]
        clip = 1.0 / jnp.sqrt(1.0 + total / entries)
        for i in range(n):
            code = low_v[i].astype(jnp.float32)
            rate = clip * code[high:high + 1, :1] * (1.0 / LOW_RATE)
            for part, at, mean, square, mean_next, square_next in (
                (code[:high], slice(i * high, (i + 1) * high), vm, vs, vm_next, vs_next),
                (low_o[i].astype(jnp.float32), slice(i * high_o, (i + 1) * high_o), om, os, om_next, os_next),
            ):
                scaled = rate * jnp.log2(part)
                mean_next[at] = 0.8 * mean[at] + 0.2 * scaled
                square_next[at] = 0.9 * square[at] + 0.1 * scaled * scaled
        split_norm(vm_next[...] / jnp.sqrt(vs_next[...] + 0.1), norms_v)
        split_norm(om_next[...] / jnp.sqrt(os_next[...] + 0.1), norms_o)
        v_step[...] = value_steps(vb[...], norms_v)
        v_next[...] = vw[...] - 0.02 * v_step[...]
        o_step[...] = output_steps(ob[...], norms_o)
        o_next[...] = ow[...] - 0.02 * o_step[...]

    count, rows, cols = wv.shape[0], wv.shape[1], wo.shape[2]
    for k in range(count):
        old = jnp.log2(wv[k].astype(jnp.float32)) * (1.0 / VALUE_RATE)
        v_copy[k * rows:(k + 1) * rows, :] = (old - 0.02 * value_steps(bases[0, k], norms_v)).astype(v_copy.dtype)
        old = jnp.log2(wo[k].astype(jnp.float32)) * (1.0 / OUTPUT_RATE)
        o_copy[:, k * cols:(k + 1) * cols] = (old - 0.02 * output_steps(bases[1, k], norms_o)).astype(o_copy.dtype)


def on_device(
    block_input,
    value_cotangent,
    mixed_output,
    output_cotangent,
    value_weight,
    output_weight,
    value_basis,
    output_basis,
    value_mean,
    value_square,
    output_mean,
    output_square,
):
    n = lax.axis_size("fs")
    depth, rank = value_basis.shape
    width = value_cotangent.shape[1]
    bases, wv, wo, low_v, low_o, sums = low_and_weights(
        block_input, value_cotangent, mixed_output, output_cotangent, value_basis, output_basis,
        value_weight, output_weight)
    entries = 2.0 * rank * width * lax.axis_size("tp")
    count = math.gcd(n, max(1, BLOCK_LANES // depth))

    def full(array):
        return pl.BlockSpec(array.shape, lambda i: (0,) * array.ndim)

    f32, b16 = jnp.float32, jnp.bfloat16
    small = [low_v, low_o, sums, value_mean, value_square, output_mean, output_square,
             value_weight, output_weight, value_basis, output_basis]
    v_row, v_small = jax.ShapeDtypeStruct((depth, width), f32), jax.ShapeDtypeStruct((rank, width), f32)
    o_row, o_small = jax.ShapeDtypeStruct((width, depth), f32), jax.ShapeDtypeStruct((width, rank), f32)
    v_all, o_all = jax.ShapeDtypeStruct((n * depth, width), b16), jax.ShapeDtypeStruct((width, n * depth), b16)
    return pl.pallas_call(
        functools.partial(epilogue, entries),
        grid=(n // count,),
        out_shape=(v_row, v_all, v_row, v_small, v_small, o_row, o_all, o_row, o_small, o_small),
        in_specs=[full(array) for array in small] + [
            pl.BlockSpec((2, count, depth, rank), lambda i: (0, i, 0, 0)),
            pl.BlockSpec((count, depth, width), lambda i: (i, 0, 0)),
            pl.BlockSpec((count, width, depth), lambda i: (i, 0, 0)),
        ],
        out_specs=[
            full(v_row), pl.BlockSpec((count * depth, width), lambda i: (i, 0)), full(v_row), full(v_small), full(v_small),
            full(o_row), pl.BlockSpec((width, count * depth), lambda i: (0, i)), full(o_row), full(o_small), full(o_small),
        ],
        scratch_shapes=[pltpu.VMEM((2, rank, width), b16), pltpu.VMEM((2, width, rank), b16)],
        compiler_params=pltpu.CompilerParams(
            dimension_semantics=("arbitrary",), vmem_limit_bytes=60 * 1024 * 1024),
    )(*small, bases, wv, wo)


def solution(mesh):
    placed = (
        P("fs", None),
        P("fs", "tp"),
        P("fs", "tp"),
        P("fs", None),
        P("fs", "tp"),
        P("tp", "fs"),
        P("fs", None),
        P("fs", None),
        P(None, "tp"),
        P(None, "tp"),
        P("tp", None),
        P("tp", None),
    )
    return jax.shard_map(
        on_device,
        mesh=mesh,
        in_specs=placed,
        out_specs=(
            P("fs", "tp"),
            P(None, "tp"),
            P("fs", "tp"),
            P(None, "tp"),
            P(None, "tp"),
            P("tp", "fs"),
            P("tp", None),
            P("tp", "fs"),
            P("tp", None),
            P("tp", None),
        ),
        check_vma=False,
    )
```

```python
import functools
import math

import jax
import jax.numpy as jnp
from jax import lax
from jax.experimental import pallas as pl
from jax.experimental.pallas import tpu as pltpu
from jax.sharding import PartitionSpec as P

MESH = pl.DeviceIdType.MESH
VALUE_RATE = 125.0 / 0.125
OUTPUT_RATE = 125.0 / 0.1875
LOW_RATE = 124.0
BLOCK_LANES = 256
TOKEN_TILE = 256


def split_fs(n):
    inner = 2 if n % 2 == 0 else 1
    middle = 2 if n % (2 * inner) == 0 else 1
    return n // (inner * middle), middle, inner


class Place:
    def __init__(self, n):
        self.sizes = split_fs(n)
        self.me = lax.axis_index("fs")
        self.core = lax.axis_index("tp")
        self.par = lax.rem(self.core, 2)
        _, b, c = self.sizes
        self.z = self.me // (b * c)
        self.y = lax.rem(self.me // c, b)
        self.x = lax.rem(self.me, c)

    def at(self, dz, ds, dt, par=None):
        a, b, c = self.sizes
        par = self.par if par is None else par
        dy = ds * (1 - par) + dt * par
        dx = ds * par + dt * (1 - par)
        z = lax.rem(self.z + dz + a, a)
        y = lax.rem(self.y + dy, b)
        x = lax.rem(self.x + dx, c)
        return (z * b + y) * c + x


class Gather:
    def __init__(self, place, slots, send, recv):
        self.p, self.slots, self.send, self.recv = place, slots, send, recv
        self.a = place.sizes[0]
        self.started = []

    def copy(self, j, src, to, sid, rid):
        ref = self.slots[j](src)
        return pltpu.make_async_remote_copy(
            src_ref=ref, dst_ref=ref, send_sem=self.send.at[j, sid], recv_sem=self.recv.at[j, rid],
            device_id={"fs": to}, device_id_type=MESH)

    def rel(self, dz, ds, dt):
        return (dz * 2 + ds) * 2 + dt

    def go(self, j, src, to, sid, rid):
        c = self.copy(j, src, to, sid, rid)
        c.start()
        self.started.append(c)

    def arrive(self, dz, ds, dt):
        for j in range(len(self.slots)):
            src = self.p.at(-dz, ds, dt)
            self.copy(j, src, self.p.me, 0, self.rel(dz, ds, dt)).wait_recv()

    def to_s(self, dz):
        for j in range(len(self.slots)):
            self.go(j, self.p.at(-dz, 0, 0), self.p.at(0, 1, 0), self.a + dz, self.rel(dz, 1, 0))

    def to_t(self, dz, ds):
        for j in range(len(self.slots)):
            self.go(j, self.p.at(-dz, ds, 0), self.p.at(0, 0, 1), 2 * self.a + dz * 2 + ds, self.rel(dz, ds, 1))

    def begin(self):
        self.begin_z()
        self.begin_st()

    def begin_z(self):
        for dz in range(1, self.a):
            for j in range(len(self.slots)):
                self.go(j, self.p.me, self.p.at(dz, 0, 0), dz, self.rel(dz, 0, 0))

    def begin_st(self):
        self.to_s(0)
        self.to_t(0, 0)

    def stage_z(self, seen=lambda *k: None):
        for dz in range(1, self.a):
            self.arrive(dz, 0, 0)
            self.to_s(dz)
            self.to_t(dz, 0)
            seen(dz, 0, 0)

    def stage_s(self, seen=lambda *k: None):
        for dz in range(self.a):
            self.arrive(dz, 1, 0)
            self.to_t(dz, 1)
            seen(dz, 1, 0)

    def stage_t(self, seen=lambda *k: None):
        for dz in range(self.a):
            for ds in range(2):
                self.arrive(dz, ds, 1)
                seen(dz, ds, 1)

    def finish(self):
        for c in self.started:
            c.wait_send()


def exchange(n, scaling, x_hbm, v_hbm, m_hbm, o_hbm, vb_ref, ob_ref, vw_ref, ow_ref,
             bases, wv, wo, low_v, low_o, sums,
             vw32, ow32, x_ref, v_ref, m_ref, o_ref, acc_v, acc_o, part_v, part_o, got_v, got_o,
             load_sem, own_sem, b_send, b_recv, c_send, c_recv, w_send, w_recv, l_send, l_recv, r_send, r_recv, q_send, q_recv):
    p = Place(n)
    a = p.sizes[0]
    par, me = p.par, p.me
    loads = [pltpu.make_async_copy(s, d, load_sem.at[i]) for i, (s, d) in enumerate(
        ((vw_ref, vw32), (ow_ref, ow32), (x_hbm, x_ref), (v_hbm, v_ref), (o_hbm, o_ref), (m_hbm, m_ref)))]
    own = [pltpu.make_async_copy(s, d, own_sem.at[i]) for i, (s, d) in enumerate(
        ((vb_ref, bases.at[0, me]), (ob_ref, bases.at[1, me])))]
    for c in own + loads:
        c.start()
    partner = p.core + 1 - 2 * par
    barrier = pltpu.get_barrier_semaphore()
    peers = [p.at(dz, 0, 0) for dz in range(1, a)] + [p.at(0, 1, 0), p.at(0, 0, 1)]
    for to in peers:
        pl.semaphore_signal(barrier, inc=1, device_id={"fs": to}, device_id_type=MESH)
    cores = lax.axis_size("tp")
    siblings = [lax.rem(p.core + d, cores) for d in range(1, cores)]
    for to in siblings:
        pl.semaphore_signal(barrier, inc=1, device_id={"tp": to}, device_id_type=MESH)
    pl.semaphore_wait(barrier, len(peers) + len(siblings))
    for c in own:
        c.wait()

    crossed = []

    def cross(dz, ds, dt):
        k = (dz * 2 + ds) * 2 + dt
        ref = bases.at[par, p.at(-dz, ds, dt)]
        c = pltpu.make_async_remote_copy(
            src_ref=ref, dst_ref=ref, send_sem=c_send.at[k], recv_sem=c_recv.at[k],
            device_id={"tp": partner}, device_id_type=MESH)
        c.start()
        crossed.append(c)

    gb = Gather(p, [lambda i: bases.at[par, i]], b_send, b_recv)
    gb.begin()
    for c in loads[:2]:
        c.wait()
    wv[me] = jnp.exp2(VALUE_RATE * vw32[...]).astype(wv.dtype)
    wo[me] = jnp.exp2(OUTPUT_RATE * ow32[...]).astype(wo.dtype)
    gb.stage_z(cross)
    gw = Gather(p, [lambda i: wv.at[i], lambda i: wo.at[i]], w_send, w_recv)
    gw.begin_z()
    gb.stage_s(cross)
    gb.stage_t(cross)
    gw.begin_st()
    for dz in range(a):
        for ds in range(2):
            for dt in range(2):
                k = (dz * 2 + ds) * 2 + dt
                if k:
                    ref = bases.at[1 - par, p.at(-dz, ds, dt, 1 - par)]
                    pltpu.make_async_remote_copy(
                        src_ref=ref, dst_ref=ref, send_sem=c_send.at[k], recv_sem=c_recv.at[k],
                        device_id={"tp": partner}, device_id_type=MESH).wait_recv()
    for c in loads[2:]:
        c.wait()

    depth, rank = bases.shape[2], bases.shape[3]
    tokens = x_ref.shape[0]
    tile = math.gcd(tokens, TOKEN_TILE)
    acc_v[...] = jnp.zeros_like(acc_v)
    acc_o[...] = jnp.zeros_like(acc_o)
    whole_v = bases[0].reshape(n * depth, rank)
    whole_o = bases[1].reshape(n * depth, rank)
    first = (((0,), (0,)), ((), ()))

    def halves(value):
        high = value.astype(jnp.bfloat16)
        return high, (value - high.astype(jnp.float32)).astype(jnp.bfloat16)

    @pl.loop(0, tokens // tile)
    def _(step):
        rows = pl.ds(pl.multiple_of(step * tile, tile), tile)
        cot = v_ref[rows, :]
        for half in halves(jnp.dot(x_ref[rows, :], whole_v, preferred_element_type=jnp.float32)):
            acc_v[...] += lax.dot_general(half, cot, first, preferred_element_type=jnp.float32)
        mixed = m_ref[rows, :]
        for half in halves(jnp.dot(o_ref[rows, :], whole_o, preferred_element_type=jnp.float32)):
            acc_o[...] += lax.dot_general(mixed, half, first, preferred_element_type=jnp.float32)

    parts, gots = (part_v, part_o), (got_v, got_o)
    for part, acc in ((part_v, acc_v), (part_o, acc_o)):
        high = part.shape[1]
        for i in range(n):
            part[i] = acc[i * high:(i + 1) * high, :] * scaling

    sent = []

    def hand(block, to, slot):
        for j in range(2):
            c = pltpu.make_async_remote_copy(
                src_ref=parts[j].at[block], dst_ref=gots[j].at[slot],
                send_sem=r_send.at[j, slot], recv_sem=r_recv.at[j, slot],
                device_id={"fs": to}, device_id_type=MESH)
            c.start()
            sent.append(c)

    def take(block, slot):
        for j in range(2):
            pltpu.make_async_remote_copy(
                src_ref=parts[j].at[block], dst_ref=gots[j].at[slot],
                send_sem=r_send.at[j, slot], recv_sem=r_recv.at[j, slot],
                device_id={"fs": me}, device_id_type=MESH).wait_recv()
            parts[j][block] += gots[j][slot]

    order = list(range(1, a)) + [0]
    for dz in order:
        for ds in (1, 0):
            hand(p.at(dz, ds, 1), p.at(0, 0, 1), dz * 2 + ds)
    gw.stage_z()
    for dz in order:
        take(p.at(dz, 1, 0), dz * 2 + 1)
        hand(p.at(dz, 1, 0), p.at(0, 1, 0), 2 * a + dz)
        take(p.at(dz, 0, 0), dz * 2)
    for dz in order:
        take(p.at(dz, 0, 0), 2 * a + dz)
        if dz:
            hand(p.at(dz, 0, 0), p.at(dz, 0, 0), 3 * a + dz)
    for dz in range(1, a):
        take(me, 3 * a + dz)
    mine_v, mine_o = part_v[me], part_o[me]

    def one(reduce, value):
        return reduce(reduce(value, axis=1, keepdims=True), axis=0, keepdims=True)

    top = jnp.maximum(one(jnp.max, jnp.abs(mine_v)), one(jnp.max, jnp.abs(mine_o)))
    top = jnp.maximum(top * 1.01, 1e-30).astype(low_v.dtype)
    square = one(jnp.sum, mine_v * mine_v) + one(jnp.sum, mine_o * mine_o)
    rate = LOW_RATE / top.astype(jnp.float32)
    high = mine_v.shape[0]
    pad = low_v.shape[1] - high
    square_high, square_low = halves(square)
    row = lax.broadcasted_iota(jnp.int32, (pad, mine_v.shape[1]), 0)
    extra = jnp.where(row == 0, top.astype(jnp.float32), jnp.where(
        row == 1, square_high.astype(jnp.float32), square_low.astype(jnp.float32)))
    low_v[me] = jnp.concatenate([jnp.exp2(rate * mine_v), extra], axis=0).astype(low_v.dtype)
    low_o[me] = jnp.exp2(rate * mine_o).astype(low_o.dtype)
    gl = Gather(p, [lambda i: low_v.at[i], lambda i: low_o.at[i]], l_send, l_recv)
    gl.begin()
    gw.stage_s()
    gl.stage_z()
    gl.stage_s()
    gl.stage_t()
    total = jnp.zeros((1, 128), jnp.float32)
    for i in range(n):
        tail = low_v[i].astype(jnp.float32)
        total += tail[high + 1:high + 2, :128] + tail[high + 2:high + 3, :128]
    sums[p.core] = jnp.broadcast_to(total, sums.shape[1:])
    for d, to in enumerate(siblings):
        c = pltpu.make_async_remote_copy(
            src_ref=sums.at[p.core], dst_ref=sums.at[p.core], send_sem=q_send.at[d], recv_sem=q_recv.at[d],
            device_id={"tp": to}, device_id_type=MESH)
        c.start()
        sent.append(c)
    gw.stage_t()
    for d in range(cores - 1):
        ref = sums.at[lax.rem(p.core - d - 1 + cores, cores)]
        pltpu.make_async_remote_copy(
            src_ref=ref, dst_ref=ref, send_sem=q_send.at[d], recv_sem=q_recv.at[d],
            device_id={"tp": partner}, device_id_type=MESH).wait_recv()
    for c in crossed + sent:
        c.wait_send()
    gb.finish()
    gw.finish()
    gl.finish()


def low_and_weights(block_input, value_cotangent, mixed_output, output_cotangent, value_basis, output_basis, value_weight, output_weight):
    n = lax.axis_size("fs")
    depth, rank = value_basis.shape
    tokens, width = value_cotangent.shape
    wide = block_input.shape[1]
    a = split_fs(n)[0]
    cores = lax.axis_size("tp")
    scaling = 1.0 / math.sqrt(tokens * n)
    f32, b16 = jnp.float32, jnp.bfloat16
    rv, ro = rank // n, width // n
    vmem = pl.BlockSpec(memory_space=pltpu.VMEM)
    hbm = pl.BlockSpec(memory_space=pl.ANY)
    dma = pltpu.SemaphoreType.DMA
    return pl.pallas_call(
        functools.partial(exchange, n, scaling),
        out_shape=(
            jax.ShapeDtypeStruct((2, n, depth, rank), b16),
            jax.ShapeDtypeStruct((n,) + value_weight.shape, b16),
            jax.ShapeDtypeStruct((n,) + output_weight.shape, b16),
            jax.ShapeDtypeStruct((n, (rv + 18) // 16 * 16, width), b16),
            jax.ShapeDtypeStruct((n, ro, rank), b16),
            jax.ShapeDtypeStruct((cores, 8, 128), f32),
        ),
        in_specs=[hbm] * 4 + [hbm] * 4,
        out_specs=[vmem] * 6,
        scratch_shapes=[
            pltpu.VMEM(value_weight.shape, f32), pltpu.VMEM(output_weight.shape, f32),
            pltpu.VMEM((tokens, wide), b16), pltpu.VMEM((tokens, width), b16),
            pltpu.VMEM((tokens, width), b16), pltpu.VMEM((tokens, wide), b16),
            pltpu.VMEM((rank, width), f32), pltpu.VMEM((width, rank), f32),
            pltpu.VMEM((n, rv, width), f32), pltpu.VMEM((n, ro, rank), f32),
            pltpu.VMEM((4 * a, rv, width), f32), pltpu.VMEM((4 * a, ro, rank), f32),
            dma((6,)), dma((2,)),
            dma((1, 4 * a)), dma((1, 4 * a)), dma((4 * a,)), dma((4 * a,)),
            dma((2, 4 * a)), dma((2, 4 * a)), dma((2, 4 * a)), dma((2, 4 * a)), dma((2, 4 * a)), dma((2, 4 * a)),
            dma((cores,)), dma((cores,)),
        ],
        compiler_params=pltpu.CompilerParams(
            collective_id=0, has_side_effects=True, vmem_limit_bytes=60 * 1024 * 1024),
    )(block_input, value_cotangent, mixed_output, output_cotangent, value_basis, output_basis, value_weight, output_weight)


def split_norm(norm, norms):
    norms[0] = norm.astype(jnp.bfloat16)
    norms[1] = (norm - norms[0].astype(jnp.float32)).astype(jnp.bfloat16)


def value_steps(basis, norms):
    return (jnp.dot(basis, norms[0], preferred_element_type=jnp.float32)
            + jnp.dot(basis, norms[1], preferred_element_type=jnp.float32))


def output_steps(basis, norms):
    last = (((1,), (1,)), ((), ()))
    return (lax.dot_general(norms[0], basis, last, preferred_element_type=jnp.float32)
            + lax.dot_general(norms[1], basis, last, preferred_element_type=jnp.float32))


def epilogue(entries, low_v, low_o, sums, vm, vs, om, os, vw, ow, vb, ob, bases, wv, wo,
             v_next, v_copy, v_step, vm_next, vs_next, o_next, o_copy, o_step, om_next, os_next,
             norms_v, norms_o):
    @pl.when(pl.program_id(0) == 0)
    def _():
        n, high, high_o = low_v.shape[0], vm.shape[0] // low_v.shape[0], low_o.shape[1]
        total = sums[0, :1, :1]
        for i in range(1, sums.shape[0]):
            total += sums[i, :1, :1]
        clip = 1.0 / jnp.sqrt(1.0 + total / entries)
        for i in range(n):
            code = low_v[i].astype(jnp.float32)
            rate = clip * code[high:high + 1, :1] * (1.0 / LOW_RATE)
            for part, at, mean, square, mean_next, square_next in (
                (code[:high], slice(i * high, (i + 1) * high), vm, vs, vm_next, vs_next),
                (low_o[i].astype(jnp.float32), slice(i * high_o, (i + 1) * high_o), om, os, om_next, os_next),
            ):
                scaled = rate * jnp.log2(part)
                mean_next[at] = 0.8 * mean[at] + 0.2 * scaled
                square_next[at] = 0.9 * square[at] + 0.1 * scaled * scaled
        split_norm(vm_next[...] / jnp.sqrt(vs_next[...] + 0.1), norms_v)
        split_norm(om_next[...] / jnp.sqrt(os_next[...] + 0.1), norms_o)
        v_step[...] = value_steps(vb[...], norms_v)
        v_next[...] = vw[...] - 0.02 * v_step[...]
        o_step[...] = output_steps(ob[...], norms_o)
        o_next[...] = ow[...] - 0.02 * o_step[...]

    count, rows, cols = wv.shape[0], wv.shape[1], wo.shape[2]
    for k in range(count):
        old = jnp.log2(wv[k].astype(jnp.float32)) * (1.0 / VALUE_RATE)
        v_copy[k * rows:(k + 1) * rows, :] = (old - 0.02 * value_steps(bases[0, k], norms_v)).astype(v_copy.dtype)
        old = jnp.log2(wo[k].astype(jnp.float32)) * (1.0 / OUTPUT_RATE)
        o_copy[:, k * cols:(k + 1) * cols] = (old - 0.02 * output_steps(bases[1, k], norms_o)).astype(o_copy.dtype)


def on_device(
    block_input,
    value_cotangent,
    mixed_output,
    output_cotangent,
    value_weight,
    output_weight,
    value_basis,
    output_basis,
    value_mean,
    value_square,
    output_mean,
    output_square,
):
    n = lax.axis_size("fs")
    depth, rank = value_basis.shape
    width = value_cotangent.shape[1]
    bases, wv, wo, low_v, low_o, sums = low_and_weights(
        block_input, value_cotangent, mixed_output, output_cotangent, value_basis, output_basis,
        value_weight, output_weight)
    entries = 2.0 * rank * width * lax.axis_size("tp")
    count = math.gcd(n, max(1, BLOCK_LANES // depth))

    def full(array):
        return pl.BlockSpec(array.shape, lambda i: (0,) * array.ndim)

    f32, b16 = jnp.float32, jnp.bfloat16
    small = [low_v, low_o, sums, value_mean, value_square, output_mean, output_square,
             value_weight, output_weight, value_basis, output_basis]
    v_row, v_small = jax.ShapeDtypeStruct((depth, width), f32), jax.ShapeDtypeStruct((rank, width), f32)
    o_row, o_small = jax.ShapeDtypeStruct((width, depth), f32), jax.ShapeDtypeStruct((width, rank), f32)
    v_all, o_all = jax.ShapeDtypeStruct((n * depth, width), b16), jax.ShapeDtypeStruct((width, n * depth), b16)
    return pl.pallas_call(
        functools.partial(epilogue, entries),
        grid=(n // count,),
        out_shape=(v_row, v_all, v_row, v_small, v_small, o_row, o_all, o_row, o_small, o_small),
        in_specs=[full(array) for array in small] + [
            pl.BlockSpec((2, count, depth, rank), lambda i: (0, i, 0, 0)),
            pl.BlockSpec((count, depth, width), lambda i: (i, 0, 0)),
            pl.BlockSpec((count, width, depth), lambda i: (i, 0, 0)),
        ],
        out_specs=[
            full(v_row), pl.BlockSpec((count * depth, width), lambda i: (i, 0)), full(v_row), full(v_small), full(v_small),
            full(o_row), pl.BlockSpec((width, count * depth), lambda i: (0, i)), full(o_row), full(o_small), full(o_small),
        ],
        scratch_shapes=[pltpu.VMEM((2, rank, width), b16), pltpu.VMEM((2, width, rank), b16)],
        compiler_params=pltpu.CompilerParams(
            dimension_semantics=("arbitrary",), vmem_limit_bytes=60 * 1024 * 1024),
    )(*small, bases, wv, wo)


def solution(mesh):
    placed = (
        P("fs", None),
        P("fs", "tp"),
        P("fs", "tp"),
        P("fs", None),
        P("fs", "tp"),
        P("tp", "fs"),
        P("fs", None),
        P("fs", None),
        P(None, "tp"),
        P(None, "tp"),
        P("tp", None),
        P("tp", None),
    )
    return jax.shard_map(
        on_device,
        mesh=mesh,
        in_specs=placed,
        out_specs=(
            P("fs", "tp"),
            P(None, "tp"),
            P("fs", "tp"),
            P(None, "tp"),
            P(None, "tp"),
            P("tp", "fs"),
            P("tp", None),
            P("tp", "fs"),
            P("tp", None),
            P("tp", None),
        ),
        check_vma=False,
    )
```
